32 devices in a mesh: kv: 8 (over z, x), tp: 4 (over y, core).
Axes of the slice: x: 2, y: 2, z: 4, core: 2. Of those that a mesh axis runs over, the one named last changes fastest.
Arguments:
- tokens: bfloat16 [96, 2048], P('tp', 'kv'), may hold values from -10.5 to 10.5
- norm_gain: float32 [2048], P('kv'), may hold values from 0.1 to 1.9
- w_query: bfloat16 [2048, 2048], P('kv', 'tp'), may hold values from -0.125 to 0.125
- w_forget: bfloat16 [2048, 2048], P('kv', 'tp'), may hold values from -0.125 to 0.125
- w_input: bfloat16 [2048, 2048], P('kv', 'tp'), may hold values from -0.125 to 0.125
- w_gate: bfloat16 [2048, 2048], P('kv', 'tp'), may hold values from -0.125 to 0.125
- lower_bound: float32 [2048], P('tp'), may hold values from 0 to 0.9
- head_gain: float32 [16, 128], P('tp'), may hold values from 0.1 to 1.9
- recur_state: float32 [96, 16, 128, 128], P('kv', 'tp'), may hold values from -3 to 3
- w_out: bfloat16 [2048, 2048], P('tp', 'kv'), may hold values from -0.125 to 0.125
- mixer_gain: float32 [2048], P('kv'), may hold values from 0.1 to 1.9
- w_up: bfloat16 [2048, 8192], P('kv', 'tp'), may hold values from -0.125 to 0.125
- w_down: bfloat16 [8192, 2048], P('tp', 'kv'), may hold values from -0.0625 to 0.0625
Outputs:
- next_tokens: bfloat16 [96, 2048], P('tp', 'kv')
- next_state: float32 [96, 16, 128, 128], P('kv', 'tp')
The draws below stay inside these ranges and needn't reach their ends.
All inputs are finite; a program needn't handle non-finite values.
Results may differ from the reference program's by a relative error of at most 0.03.
Values may be sent and summed in bfloat16 or wider, within the bound.
A program may use at most 64 MiB of HBM per device.

```python
import jax
import jax.numpy as jnp
from jax import lax

D = 2048
HEADS = 16
KEY = 128
VAL = 128
FF = 8192
SEQS = 96
N_TP = 4


def draw_tokens(key, part):
    first_key = jax.random.fold_in(key, 11)
    column = jnp.arange(D, dtype=jnp.float32) / D - 0.5
    base_draw = jnp.clip(jax.random.normal(first_key, (SEQS, D), jnp.float32), -6.0, 6.0)
    values = base_draw * jnp.exp(jnp.log(3.0) * column)[None, :]
    return values.astype(jnp.bfloat16)


def block_scale(own_key, shape, pieces, least, high):
    factor_of, own = 1.0, jax.random.fold_in(own_key, 6)
    for axis_at, parts in pieces:
        heights = jnp.exp(jax.random.uniform(jax.random.fold_in(own, axis_at), (parts,), jnp.float32, least / len(pieces), high / len(pieces)))
        factor_of = factor_of * jnp.repeat(heights, shape[axis_at] // parts).reshape([-1 if axis == axis_at else 1 for axis in range(len(shape))])
    return factor_of


def noise(key, dims, width, most, split=(), held_as=jnp.bfloat16):
    drawn = width * jax.random.normal(key, dims, jnp.float32)
    if split:
        drawn = drawn * block_scale(key, dims, split, -0.22, 0.18)
    return jnp.clip(drawn, -most, most).astype(held_as)


def setup_inputs(seed: int = 0) -> dict:
    key_list = jax.random.split(jax.random.key(seed), 14)
    return {
        "tokens": draw_tokens(jax.random.fold_in(key_list[13], 71), 0),
        "norm_gain": jnp.clip(1.0 + 0.18 * jax.random.normal(key_list[1], (D,), jnp.float32), 0.1, 1.9),
        "w_query": noise(key_list[2], (D, HEADS * KEY), D ** -0.5, 0.125, ((0, 8), (1, 4))),
        "w_forget": noise(key_list[3], (D, HEADS * KEY), D ** -0.5, 0.125, ((0, 8), (1, 4))),
        "w_input": noise(key_list[4], (D, HEADS * VAL), D ** -0.5, 0.125, ((0, 8), (1, 4))),
        "w_gate": noise(key_list[5], (D, HEADS * VAL), D ** -0.5, 0.125, ((0, 8), (1, 4))),
        "lower_bound": jnp.clip(0.9 * jax.random.uniform(key_list[6], (HEADS * KEY,), jnp.float32) ** block_scale(key_list[6], (HEADS * KEY,), ((0, 4),), -0.2, 0.2), 0.0, 0.9),
        "head_gain": jnp.clip(1.0 + 0.18 * jax.random.normal(key_list[7], (HEADS, VAL), jnp.float32), 0.1, 1.9),
        "recur_state": noise(key_list[8], (SEQS, HEADS, KEY, VAL), 0.5, 3.0, ((0, 8), (1, 4)), jnp.float32),
        "w_out": noise(key_list[9], (HEADS * VAL, D), (HEADS * VAL) ** -0.5, 0.125, ((0, 4), (1, 8))),
        "mixer_gain": jnp.clip(1.0 + 0.18 * jax.random.normal(key_list[10], (D,), jnp.float32), 0.1, 1.9),
        "w_up": noise(key_list[11], (D, FF), D ** -0.5, 0.125, ((0, 8), (1, 4))),
        "w_down": noise(key_list[12], (FF, D), FF ** -0.5, 0.0625, ((0, 4), (1, 8))),
    }


NORM_EPS = 1e-05

def project(row_block, norm_scale, weight):
    tokens_f = row_block.astype(jnp.float32)
    row_scale = lax.rsqrt(lax.optimization_barrier(jnp.mean(tokens_f * tokens_f, axis=1)) + NORM_EPS)
    normed = (tokens_f * norm_scale).astype(jnp.bfloat16)
    return jnp.dot(normed, weight, preferred_element_type=jnp.float32) * row_scale[:, None]

def grouped(values_bf, weight):
    count = values_bf.shape[0]
    grouped_vals = values_bf.reshape(count, N_TP, -1).astype(jnp.float32)
    grouped_mats = weight.reshape(N_TP, -1, weight.shape[1]).astype(jnp.float32)
    partials = jnp.einsum('rgc,gcd->grd', grouped_vals, grouped_mats)
    return lax.optimization_barrier(jnp.sum(partials.astype(jnp.bfloat16).astype(jnp.float32), axis=0))

def reference(tokens, norm_gain, w_query, w_forget, w_input, w_gate, lower_bound, head_gain, recur_state, w_out, mixer_gain, w_up, w_down):
    count = tokens.shape[0]
    queries = project(tokens, norm_gain, w_query).reshape(count, HEADS, KEY)
    forget_raw = project(tokens, norm_gain, w_forget).reshape(count, HEADS, KEY)
    values_in = project(tokens, norm_gain, w_input).reshape(count, HEADS, VAL)
    gate_raw = project(tokens, norm_gain, w_gate)
    bound = lower_bound.reshape(HEADS, KEY)
    forget = bound + (1.0 - bound) * jax.nn.sigmoid(forget_raw)
    next_state = forget[..., None] * recur_state + (1.0 - forget)[..., None] * values_in[:, :, None, :]
    read_out = jnp.einsum('rhk,rhkv->rhv', queries, next_state, precision=lax.Precision.HIGHEST)
    read_out = read_out * lax.rsqrt(lax.optimization_barrier(jnp.mean(read_out * read_out, axis=2, keepdims=True)) + NORM_EPS) * head_gain
    mixture = (read_out.reshape(count, HEADS * VAL) * jax.nn.silu(gate_raw)).astype(jnp.bfloat16)
    mixed_rows = (tokens.astype(jnp.float32) + grouped(mixture, w_out)).astype(jnp.bfloat16)
    hidden_pre = project(mixed_rows, mixer_gain, w_up)
    hidden = jnp.square(jax.nn.relu(hidden_pre)).astype(jnp.bfloat16)
    next_tokens = (mixed_rows.astype(jnp.float32) + grouped(hidden, w_down)).astype(jnp.bfloat16)
    return (next_tokens, next_state)
```

```python
import functools

import jax
import jax.numpy as jnp
from jax import lax
from jax.experimental import pallas as pl
from jax.experimental.pallas import tpu as pltpu
from jax.sharding import PartitionSpec as P

NORM_EPS = 1e-05
F32 = jnp.float32
BF16 = jnp.bfloat16


def round_up(value, step):
    return (value + step - 1) // step * step


def remote(src, dst, send_sem, recv_sem, axis, peer):
    return pltpu.make_async_remote_copy(
        src_ref=src,
        dst_ref=dst,
        send_sem=send_sem,
        recv_sem=recv_sem,
        device_id={axis: peer},
        device_id_type=pl.DeviceIdType.MESH,
    )


def kernel(
    n_kv,
    n_tp,
    tok_hbm,
    gain_hbm,
    wq_hbm,
    wf_hbm,
    wi_hbm,
    wg_hbm,
    bound_hbm,
    hgain_hbm,
    state_hbm,
    wo_hbm,
    mgain_hbm,
    wu_hbm,
    wd_hbm,
    out_ref,
    ns_ref,
    gain_ref,
    bound_ref,
    hgain_ref,
    mgain_ref,
    w_in,
    wo,
    wu,
    wd,
    state,
    state_bf,
    tokbuf,
    send2,
    pair2,
    out2,
    recv2,
    sq_send,
    sq_recv,
    mix_send,
    mix_recv,
    send4,
    recv4,
    mixed_buf,
    send5,
    pair5,
    out5,
    recv5,
    sq5_send,
    sq5_recv,
    hid_send,
    hid_recv,
    send7,
    recv7,
    load_sem,
    send_sem,
    tp_recv_sem,
    sq_recv_sem,
    mix_recv_sem,
    pair_recv_sem,
    far_recv_sem,
    hid_recv_sem,
):
    kv = lax.axis_index("kv")
    tp = lax.axis_index("tp")
    row_block, feats = tok_hbm.shape
    rows = row_block * n_tp
    own, heads, key, val = state_hbm.shape
    span = heads * key
    pad_rows = sq_send.shape[1]
    chunk = send5.shape[2]
    width = feats * n_kv
    half_rows = rows // 2
    half_blocks = n_tp // 2
    n_far = n_kv // 2
    far, near = kv // 2, lax.rem(kv, 2)
    partner = 2 * far + 1 - near
    if n_far == 4:
        far_peers = [3 - far, lax.rem(far + 2, 4), far + 1 - 2 * lax.rem(far, 2)]
    else:
        far_peers = [lax.rem(far + off, n_far) for off in range(1, n_far)]

    small = [
        pltpu.make_async_copy(tok_hbm, tokbuf.at[tp], load_sem.at[8]),
        pltpu.make_async_copy(gain_hbm, gain_ref, load_sem.at[9]),
        pltpu.make_async_copy(bound_hbm, bound_ref, load_sem.at[10]),
        pltpu.make_async_copy(hgain_hbm, hgain_ref, load_sem.at[11]),
        pltpu.make_async_copy(mgain_hbm, mgain_ref, load_sem.at[12]),
    ]
    for copy in small:
        copy.start()
    loads = []
    for i, src in enumerate((wq_hbm, wf_hbm, wi_hbm, wg_hbm)):
        loads.append(pltpu.make_async_copy(src, w_in.at[i], load_sem.at[i]))
    loads.append(pltpu.make_async_copy(state_hbm, state, load_sem.at[4]))
    loads.append(pltpu.make_async_copy(wo_hbm, wo, load_sem.at[5]))
    loads.append(pltpu.make_async_copy(wu_hbm, wu, load_sem.at[6]))
    loads.append(pltpu.make_async_copy(wd_hbm, wd, load_sem.at[7]))
    for copy in loads:
        copy.start()

    def kv_peer(off):
        return lax.rem(kv + off, n_kv)

    def tp_peer(off):
        return lax.rem(tp + off, n_tp)

    barrier = pltpu.get_barrier_semaphore()
    for off in range(1, n_kv):
        pl.semaphore_signal(
            barrier, inc=1, device_id={"kv": kv_peer(off)}, device_id_type=pl.DeviceIdType.MESH
        )
    for off in range(1, n_tp):
        pl.semaphore_signal(
            barrier, inc=1, device_id={"tp": tp_peer(off)}, device_id_type=pl.DeviceIdType.MESH
        )
    pl.semaphore_wait(barrier, n_kv + n_tp - 2)

    def tp_copy(phase, send_at, src, dst, peer):
        return remote(src, dst, send_sem.at[send_at], tp_recv_sem.at[phase], "tp", peer)

    def kv_copy(send_at, src, dst, recv_sem, peer):
        return remote(src, dst, send_sem.at[send_at], recv_sem, "kv", peer)

    def pair_send(phase, source, pair, half, at):
        src = source.at[half * n_kv + 2 * at + 1 - near]
        slot = half * n_far + at
        kv_copy(4 * phase + 4, src, pair.at[slot], pair_recv_sem.at[phase, slot], partner).start()

    def pair_wait(phase, pair, half, at):
        slot = half * n_far + at
        kv_copy(0, pair.at[slot], pair.at[slot], pair_recv_sem.at[phase, slot], partner).wait_recv()
        return pair[slot].astype(F32)

    def far_send(phase, out, received, half, at):
        src = out.at[half * n_far + at]
        dst = received.at[half * n_far + far]
        kv_copy(4 * phase + 5, src, dst, far_recv_sem.at[2 * phase + half], 2 * at + near).start()

    def far_wait(phase, received, half):
        block = received.at[pl.ds(half * n_far, n_far - 1)]
        kv_copy(0, block, block, far_recv_sem.at[2 * phase + half], partner).wait_recv()

    for copy in small:
        copy.wait()
    others = pl.ds(0, n_tp - 1)
    for off in range(1, n_tp):
        tp_copy(0, 0, tokbuf.at[tp], tokbuf.at[tp], tp_peer(off)).start()
    tp_copy(0, 0, tokbuf.at[others], tokbuf.at[others], tp_peer(1)).wait_recv()
    tokens = jnp.concatenate([tokbuf[t].astype(F32) for t in range(n_tp)], axis=0)

    row_at = lax.broadcasted_iota(jnp.int32, (rows, pad_rows), 0)
    col_at = lax.broadcasted_iota(jnp.int32, (rows, pad_rows), 1)
    diagonal = row_at == col_at

    def as_row(column):
        return jnp.sum(jnp.where(diagonal, column, 0.0), axis=0, keepdims=True)

    normed = (tokens * gain_ref[...]).astype(BF16)
    sq_send[...] = as_row(jnp.sum(tokens * tokens, axis=1, keepdims=True))
    sq_recv[kv] = sq_send[...]
    for half in range(2):
        parts = []
        for i in (2 * half, 2 * half + 1):
            loads[i].wait()
            parts.append(jnp.dot(normed, w_in[i], preferred_element_type=F32))
        for d in range(n_kv):
            send2[half * n_kv + d] = jnp.concatenate(
                [part[d * own : (d + 1) * own] for part in parts], axis=0
            ).astype(BF16)
        for at in far_peers + [far]:
            pair_send(0, send2, pair2, half, at)
    for off in range(1, n_kv):
        kv_copy(1, sq_send, sq_recv.at[kv], sq_recv_sem.at[0], kv_peer(off)).start()
    for half in range(2):
        for at in far_peers:
            own_part = send2[half * n_kv + 2 * at + near].astype(F32)
            out2[half * n_far + at] = (own_part + pair_wait(0, pair2, half, at)).astype(BF16)
            far_send(0, out2, recv2, half, at)
    totals = []
    for half in range(2):
        totals.append(send2[half * n_kv + kv].astype(F32) + pair_wait(0, pair2, half, far))
    loads[4].wait()
    for s in range(own):
        for h in range(heads):
            state_bf[h, :, s * val : (s + 1) * val] = state[s, h].astype(BF16)

    for half in range(2):
        far_wait(0, recv2, half)
        for at in far_peers:
            totals[half] = totals[half] + recv2[half * n_far + at].astype(F32)
    kv_others = pl.ds(0, n_kv - 1)
    kv_copy(1, sq_recv.at[kv_others], sq_recv.at[kv_others], sq_recv_sem.at[0], partner).wait_recv()
    sq_total = sq_recv[0]
    for d in range(1, n_kv):
        sq_total = sq_total + sq_recv[d]
    own_at = lax.broadcasted_iota(jnp.int32, (own, pad_rows), 0) + kv * own
    lane_at = lax.broadcasted_iota(jnp.int32, (own, pad_rows), 1)
    own_sq = jnp.sum(jnp.where(own_at == lane_at, sq_total, 0.0), axis=1, keepdims=True)
    scale = lax.rsqrt(own_sq / width + NORM_EPS)
    queries = totals[0][:own] * scale
    forget_raw = totals[0][own:] * scale
    values_in = totals[1][:own] * scale
    gate = totals[1][own:] * scale
    bound = bound_ref[...]
    forget = bound + (1.0 - bound) * jax.nn.sigmoid(forget_raw)
    decayed = queries * forget
    fresh = queries - decayed
    decayed = decayed.astype(BF16)
    seq_at = lax.broadcasted_iota(jnp.int32, (own, val), 0)
    mixture = []
    for h in range(heads):
        cols = slice(h * key, (h + 1) * key)
        vals = slice(h * val, (h + 1) * val)
        wide = jnp.dot(decayed[:, cols], state_bf[h], preferred_element_type=F32)
        read = jnp.sum(fresh[:, cols], axis=1, keepdims=True) * values_in[:, vals]
        for s in range(own):
            read = read + jnp.where(seq_at == s, wide[:, s * val : (s + 1) * val], 0.0)
        mean = jnp.mean(read * read, axis=1, keepdims=True)
        read = read * lax.rsqrt(mean + NORM_EPS) * hgain_ref[h : h + 1]
        mixture.append(read * jax.nn.silu(gate[:, vals]))
    mix_send[...] = jnp.concatenate(mixture, axis=0).astype(BF16)
    for off in range(1, n_kv):
        kv_copy(2, mix_send, mix_recv.at[kv], mix_recv_sem.at[0], kv_peer(off)).start()
    mix_recv[kv] = mix_send[...]

    for h in range(heads):
        cols = slice(h * key, (h + 1) * key)
        vals = slice(h * val, (h + 1) * val)
        fill = jnp.zeros((round_up(own, 128) - own, key), F32)
        turned = jnp.concatenate([forget[:, cols], fill], axis=0).T
        for s in range(own):
            fresh_row = values_in[s : s + 1, vals]
            ns_ref[s, h] = fresh_row + turned[:, s : s + 1] * (state[s, h] - fresh_row)

    loads[5].wait()
    kv_copy(2, mix_recv.at[kv_others], mix_recv.at[kv_others], mix_recv_sem.at[0], partner).wait_recv()
    blocks = [mix_recv[d].astype(F32) for d in range(n_kv)]
    gathered = jnp.concatenate(
        [
            jnp.concatenate([block[h * own : (h + 1) * own] for block in blocks], axis=0)
            for h in range(heads)
        ],
        axis=1,
    ).astype(BF16)
    for half in range(2):
        here = gathered[half * half_rows : (half + 1) * half_rows]
        send4[half] = jnp.dot(here, wo[...], preferred_element_type=F32).astype(BF16)
        for off in range(1, n_tp):
            tp_copy(1 + half, 3, send4.at[half], recv4.at[half * n_tp + tp], tp_peer(off)).start()
        recv4[half * n_tp + tp] = send4[half]
    loads[6].wait()
    aligned = chunk % 128 == 0

    def up(half, normed, peer):
        if not aligned:
            return send5[half * n_kv + peer].astype(F32)
        columns = pl.ds(pl.multiple_of(peer * chunk, 128), chunk)
        return jnp.dot(normed, wu[:, columns], preferred_element_type=F32)

    normed_halves = []
    squares = 0.0
    for half in range(2):
        block = recv4.at[pl.ds(half * n_tp, n_tp - 1)]
        tp_copy(1 + half, 3, block, block, tp_peer(1)).wait_recv()
        attn = recv4[half * n_tp].astype(F32)
        for t in range(1, n_tp):
            attn = attn + recv4[half * n_tp + t].astype(F32)
        blocks = range(half * half_blocks, (half + 1) * half_blocks)
        tokens = jnp.concatenate([tokbuf[t].astype(F32) for t in blocks], axis=0)
        mixed = (tokens + attn).astype(BF16).astype(F32)
        for i, t in enumerate(blocks):
            mixed_buf[t] = mixed[i * row_block : (i + 1) * row_block]
        normed = (mixed * mgain_ref[...]).astype(BF16)
        normed_halves.append(normed)
        if not aligned:
            hidden_all = jnp.dot(normed, wu[...], preferred_element_type=F32).astype(BF16)
            for c in range(n_kv):
                send5[half * n_kv + c] = hidden_all[:, c * chunk : (c + 1) * chunk]
        for at in far_peers + [far]:
            peer = 2 * at + 1 - near
            if aligned:
                send5[half * n_kv + peer] = up(half, normed, peer).astype(BF16)
            pair_send(1, send5, pair5, half, at)
        half_at = diagonal[half * half_rows : (half + 1) * half_rows]
        column = jnp.sum(mixed * mixed, axis=1, keepdims=True)
        squares = squares + jnp.sum(jnp.where(half_at, column, 0.0), axis=0, keepdims=True)
    sq5_send[...] = squares
    sq5_recv[kv] = squares
    for off in range(1, n_kv):
        kv_copy(6, sq5_send, sq5_recv.at[kv], sq_recv_sem.at[1], kv_peer(off)).start()
    for half in range(2):
        for at in far_peers:
            own_part = up(half, normed_halves[half], 2 * at + near)
            out5[half * n_far + at] = (own_part + pair_wait(1, pair5, half, at)).astype(BF16)
            far_send(1, out5, recv5, half, at)
    kv_copy(6, sq5_recv.at[kv_others], sq5_recv.at[kv_others], sq_recv_sem.at[1], partner).wait_recv()
    sq_total = sq5_recv[0]
    for d in range(1, n_kv):
        sq_total = sq_total + sq5_recv[d]
    row_sq = jnp.sum(jnp.where(diagonal, sq_total, 0.0), axis=1, keepdims=True)
    row_scale = lax.rsqrt(row_sq / width + NORM_EPS)
    for half in range(2):
        total = up(half, normed_halves[half], kv) + pair_wait(1, pair5, half, far)
        far_wait(1, recv5, half)
        for at in far_peers:
            total = total + recv5[half * n_far + at].astype(F32)
        scale = row_scale[half * half_rows : (half + 1) * half_rows]
        hidden = jnp.maximum(total * scale, 0.0)
        hid_send[half] = (hidden * hidden).astype(BF16)
        slot = half * n_kv + kv
        for peer in [2 * at + near for at in far_peers] + [partner]:
            kv_copy(7, hid_send.at[half], hid_recv.at[slot], hid_recv_sem.at[slot], peer).start()
    loads[7].wait()

    def down(source, block):
        at = pl.ds(pl.multiple_of(source * chunk, chunk), chunk)
        return jnp.dot(block, wd[at, :], preferred_element_type=F32)

    def hid_wait(half, src):
        slot = half * n_kv + src
        kv_copy(7, hid_recv.at[slot], hid_recv.at[slot], hid_recv_sem.at[slot], partner).wait_recv()

    sums = []
    for half in range(2):
        total = down(kv, hid_send[half])
        hid_wait(half, partner)
        total = total + down(partner, hid_recv[half * n_kv + partner])
        for at in reversed(far_peers):
            src = 2 * at + near
            slot = half * n_kv + src
            hid_wait(half, src)
            kv_copy(10, hid_recv.at[slot], hid_recv.at[slot], hid_recv_sem.at[slot], partner).start()
            total = total + down(src, hid_recv[slot])
        sums.append(total)
    for half in range(2):
        total = sums[half]
        for at in reversed(far_peers):
            src = 2 * at + 1 - near
            hid_wait(half, src)
            total = total + down(src, hid_recv[half * n_kv + src])
        for i in range(half_blocks):
            t = half * half_blocks + i
            send7[t] = total[i * row_block : (i + 1) * row_block].astype(BF16)

            @pl.when(t != tp)
            def _():
                tp_copy(3, 11, send7.at[t], recv7.at[tp], t).start()

    recv7[tp] = send7[tp]
    tp_copy(3, 11, recv7.at[others], recv7.at[others], tp_peer(1)).wait_recv()
    down_out = recv7[0].astype(F32)
    for t in range(1, n_tp):
        down_out = down_out + recv7[t].astype(F32)
    out_ref[...] = (mixed_buf[tp] + down_out).astype(BF16)

    def drain(send_at, buffer, count):
        block = buffer.at[pl.ds(0, count)]
        kv_copy(send_at, block, block, sq_recv_sem.at[0], partner).wait_send()

    drain(0, tokbuf, n_tp - 1)
    drain(1, sq_recv, n_kv - 1)
    drain(2, mix_recv, n_kv - 1)
    drain(3, recv4, 2 * (n_tp - 1))
    drain(4, send2, n_kv)
    drain(5, send2, n_kv - 2)
    drain(6, sq5_recv, n_kv - 1)
    drain(7, send5, n_kv)
    drain(8, send5, n_kv)
    drain(9, send5, n_kv - 2)
    drain(10, send5, n_kv - 2)
    drain(11, send7, n_tp - 1)


def store(tokens_ref, state_ref, tokens_out, state_out, sem):
    copies = [
        pltpu.make_async_copy(tokens_ref, tokens_out, sem.at[0]),
        pltpu.make_async_copy(state_ref, state_out, sem.at[1]),
    ]
    for copy in copies:
        copy.start()
    for copy in copies:
        copy.wait()


def solution(mesh):
    n_kv, n_tp = mesh.shape["kv"], mesh.shape["tp"]

    def body(
        tokens,
        norm_gain,
        w_query,
        w_forget,
        w_input,
        w_gate,
        lower_bound,
        head_gain,
        recur_state,
        w_out,
        mixer_gain,
        w_up,
        w_down,
    ):
        row_block, feats = tokens.shape
        rows = row_block * n_tp
        own, heads, key, val = recur_state.shape
        span = w_query.shape[1]
        units = w_up.shape[1]
        chunk = units // n_kv
        pad_rows = round_up(rows, 128)
        kept = recur_state.size * 4 + round_up(row_block, 16) * round_up(feats, 128) * 2
        grant = 67043328 - kept - 16384
        vmem = pl.BlockSpec(memory_space=pltpu.VMEM)
        hbm = pl.BlockSpec(memory_space=pltpu.HBM)
        next_tokens, next_state = pl.pallas_call(
            functools.partial(kernel, n_kv, n_tp),
            out_shape=(
                pltpu.VMEM(tokens.shape, BF16),
                pltpu.VMEM(recur_state.shape, F32),
            ),
            in_specs=[hbm] * 13,
            out_specs=(vmem, vmem),
            scratch_shapes=[
                pltpu.VMEM((1, feats), F32),
                pltpu.VMEM((1, span), F32),
                pltpu.VMEM(head_gain.shape, F32),
                pltpu.VMEM((1, feats), F32),
                pltpu.VMEM((4, feats, span), BF16),
                pltpu.VMEM(w_out.shape, BF16),
                pltpu.VMEM(w_up.shape, BF16),
                pltpu.VMEM(w_down.shape, BF16),
                pltpu.VMEM(recur_state.shape, F32),
                pltpu.VMEM((heads, key, own * val), BF16),
                pltpu.VMEM((n_tp, row_block, feats), BF16),
                pltpu.VMEM((2 * n_kv, 2 * own, span), BF16),
                pltpu.VMEM((n_kv, 2 * own, span), BF16),
                pltpu.VMEM((n_kv, 2 * own, span), BF16),
                pltpu.VMEM((n_kv, 2 * own, span), BF16),
                pltpu.VMEM((1, pad_rows), F32),
                pltpu.VMEM((n_kv, 1, pad_rows), F32),
                pltpu.VMEM((heads * own, val), BF16),
                pltpu.VMEM((n_kv, heads * own, val), BF16),
                pltpu.VMEM((2, rows // 2, feats), BF16),
                pltpu.VMEM((2 * n_tp, rows // 2, feats), BF16),
                pltpu.VMEM((n_tp, row_block, feats), F32),
                pltpu.VMEM((2 * n_kv, rows // 2, chunk), BF16),
                pltpu.VMEM((n_kv, rows // 2, chunk), BF16),
                pltpu.VMEM((n_kv, rows // 2, chunk), BF16),
                pltpu.VMEM((n_kv, rows // 2, chunk), BF16),
                pltpu.VMEM((1, pad_rows), F32),
                pltpu.VMEM((n_kv, 1, pad_rows), F32),
                pltpu.VMEM((2, rows // 2, chunk), BF16),
                pltpu.VMEM((2 * n_kv, rows // 2, chunk), BF16),
                pltpu.VMEM((n_tp, row_block, feats), BF16),
                pltpu.VMEM((n_tp, row_block, feats), BF16),
                pltpu.SemaphoreType.DMA((13,)),
                pltpu.SemaphoreType.DMA((12,)),
                pltpu.SemaphoreType.DMA((4,)),
                pltpu.SemaphoreType.DMA((2,)),
                pltpu.SemaphoreType.DMA((1,)),
                pltpu.SemaphoreType.DMA((2, n_kv)),
                pltpu.SemaphoreType.DMA((4,)),
                pltpu.SemaphoreType.DMA((2 * n_kv,)),
            ],
            compiler_params=pltpu.CompilerParams(collective_id=0, has_side_effects=True, vmem_limit_bytes=grant),
        )(
            tokens,
            norm_gain.reshape(1, feats),
            w_query,
            w_forget,
            w_input,
            w_gate,
            lower_bound.reshape(1, span),
            head_gain,
            recur_state,
            w_out,
            mixer_gain.reshape(1, feats),
            w_up,
            w_down,
        )
        out_shape = (
            jax.ShapeDtypeStruct(tokens.shape, BF16),
            jax.ShapeDtypeStruct(recur_state.shape, F32),
        )
        return pl.pallas_call(
            store,
            out_shape=out_shape,
            in_specs=[vmem] * 2,
            out_specs=(hbm, hbm),
            scratch_shapes=[pltpu.SemaphoreType.DMA((2,))],
            compiler_params=pltpu.CompilerParams(vmem_limit_bytes=2**20, has_side_effects=True),
        )(next_tokens, next_state)

    in_specs = (
        P("tp", "kv"),
        P("kv"),
        P("kv", "tp"),
        P("kv", "tp"),
        P("kv", "tp"),
        P("kv", "tp"),
        P("tp"),
        P("tp", None),
        P("kv", "tp", None, None),
        P("tp", "kv"),
        P("kv"),
        P("kv", "tp"),
        P("tp", "kv"),
    )
    out_specs = (P("tp", "kv"), P("kv", "tp", None, None))
    return jax.shard_map(body, mesh=mesh, in_specs=in_specs, out_specs=out_specs, check_vma=False)
```
